128 devices in a mesh: sp: 32 (over z, y, core), tp: 4 (over x).
Axes of the slice: x: 4, y: 4, z: 4, core: 2. Of those that a mesh axis runs over, the one named last changes fastest.
Arguments:
- tokens: bfloat16 [16384, 2048], P(('sp', 'tp')), may hold values from -6 to 6
- queries: bfloat16 [16384, 1024], P('sp', 'tp'), may hold values from -160 to 160
- keys: bfloat16 [16384, 1024], P('sp', 'tp'), may hold values from -8 to 8
- values: bfloat16 [16384, 1024], P('sp', 'tp'), may hold values from -6 to 6
- lambdas: float32 [8], P('tp'), may hold values from 0.3 to 0.8
- head_gain: float32 [128], replicated, may hold values from 0.1 to 1.9
- out_weight: bfloat16 [1024, 2048], replicated, may hold values from -0.1875 to 0.1875
- mixer_gain: float32 [2048], replicated, may hold values from 0.1 to 1.9
- up_weight: bfloat16 [2048, 4096], P('sp', 'tp'), may hold values from -0.125 to 0.125
- down_weight: bfloat16 [4096, 2048], P('tp', 'sp'), may hold values from -0.09375 to 0.09375
Outputs:
- result: bfloat16 [16384, 2048], P(('sp', 'tp'))
The draws below stay inside these ranges and needn't reach their ends.
All inputs are finite; a program needn't handle non-finite values.
Results may differ from the reference program's by a relative error of at most 0.02.
Values may be sent and summed in bfloat16 or wider, within the bound.
No kernel may reach another device: no remote copies, remote signals or barrier semaphores. Data moves between devices by JAX's collectives and lax.ppermute only.
A program may use at most 128 MiB of HBM per device.

```python
import math
import jax
import jax.numpy as jnp
from jax import lax

D = 2048
HEADS = 8
DQK = 64
DV = 128
ATTN = 1024
FF = 4096
TOKENS = 16384


def drawn(key):
    base = jax.random.normal(jax.random.fold_in(key, 11), (TOKENS, HEADS * 2 * DQK), jnp.float32) * 1.3
    base = jnp.clip(base, -7.8, 7.8)
    return base


def draw_keys(key, part):
    base = drawn(key)
    return base.astype(jnp.bfloat16)


def draw_queries(key, part):
    own = jax.random.normal(jax.random.fold_in(key, 21), (TOKENS, HEADS * 2 * DQK), jnp.float32) * 1.3
    own = jnp.clip(own, -7.8, 7.8)
    return own.astype(jnp.bfloat16)


def steps_of(own_key, shape, pieces, least, top_value):
    loudness = 1.0
    for position, blocks in pieces:
        steps = jax.random.uniform(jax.random.fold_in(jax.random.fold_in(own_key, 6), position), (blocks,), jnp.float32, least / len(pieces), top_value / len(pieces))
        loudness = loudness * jnp.repeat(jnp.exp(steps), shape[position] // blocks).reshape((-1,) + (1,) * (len(shape) - 1 - position))
    return loudness


def bell_draw(key, dims, width, most, cuts=(), kind=jnp.bfloat16):
    entries = jax.random.normal(key, dims, jnp.float32) * width
    if len(cuts) > 0:
        entries = steps_of(key, dims, cuts, -0.22, 0.18) * entries
    return jnp.clip(entries, min=-most, max=most).astype(kind)


def setup_inputs(seed: int = 0) -> dict:
    splits = jax.random.split(jax.random.key(seed), 11)
    tokens = bell_draw(splits[0], (TOKENS, D), 1.0, 6.0, ((0, 128),))
    queries = draw_queries(jax.random.fold_in(splits[10], 71), 0)
    keys = draw_keys(jax.random.fold_in(splits[10], 71), 0)
    values = bell_draw(splits[3], (TOKENS, ATTN), 1.0, 6.0, ((0, 32), (1, 4)))
    lambdas = jnp.clip(0.3 + 0.5 * jax.random.uniform(splits[4], (HEADS,), jnp.float32) ** steps_of(splits[4], (HEADS,), ((0, 4),), -0.2, 0.2), 0.3, 0.8)
    head_gain = jnp.clip(1.0 + 0.18 * jax.random.normal(splits[5], (DV,), jnp.float32), 0.1, 1.9)
    out_weight = bell_draw(splits[6], (ATTN, D), ATTN ** -0.5, 0.1875)
    mixer_gain = jnp.clip(1.0 + 0.18 * jax.random.normal(splits[7], (D,), jnp.float32), 0.1, 1.9)
    up_weight = bell_draw(splits[8], (D, FF), D ** -0.5, 0.125, ((0, 32), (1, 4)))
    down_weight = bell_draw(splits[9], (FF, D), FF ** -0.5, 0.09375, ((0, 4), (1, 32)))
    return {"tokens": tokens, "queries": queries, "keys": keys, "values": values, "lambdas": lambdas, "head_gain": head_gain, "out_weight": out_weight, "mixer_gain": mixer_gain, "up_weight": up_weight, "down_weight": down_weight}


def reference(tokens, queries, keys, values, lambdas, head_gain, out_weight, mixer_gain, up_weight, down_weight):
    query_heads = jnp.transpose(queries.astype(jnp.float32).reshape(TOKENS, HEADS, 2, DQK), (1, 2, 0, 3))
    key_heads = jnp.transpose(keys.astype(jnp.float32).reshape(TOKENS, HEADS, 2, DQK), (1, 2, 0, 3))
    value_heads = jnp.transpose(values.astype(jnp.float32).reshape(TOKENS, HEADS, DV), (1, 0, 2))
    block_rows = math.gcd(TOKENS, 512)
    positions = jnp.arange(TOKENS, dtype=jnp.int32)

    def one_head(inputs):
        query_pair, key_pair, value_rows, lam_value = inputs

        def one_block(block_index):
            offset = (block_index * block_rows).astype(jnp.int32)
            query_pos = offset + jnp.arange(block_rows, dtype=jnp.int32)
            allowed = positions[None, :] <= query_pos[:, None]
            head_maps = []
            for map_index in range(2):
                query_rows = lax.dynamic_slice_in_dim(query_pair[map_index], offset, block_rows, 0)
                scores = jnp.dot(query_rows, key_pair[map_index].T, precision=lax.Precision.HIGHEST, preferred_element_type=jnp.float32) * DQK ** (-0.5)
                scores = jnp.where(allowed, scores, -jnp.inf)
                row_max = lax.optimization_barrier(jnp.max(scores, axis=1, keepdims=True))
                exponent = jnp.exp(scores - row_max)
                row_total = lax.optimization_barrier(jnp.sum(exponent, axis=1, keepdims=True))
                weights = lax.optimization_barrier(exponent.astype(jnp.bfloat16)).astype(jnp.float32)
                head_maps.append(jnp.dot(weights, value_rows, precision=lax.Precision.HIGHEST, preferred_element_type=jnp.float32) / row_total)
            differ = head_maps[0] - lam_value * head_maps[1]
            spread = lax.rsqrt(lax.optimization_barrier(jnp.mean(differ * differ, axis=1, keepdims=True)) + 1e-06)
            return (differ * spread * head_gain).astype(jnp.bfloat16)
        return lax.map(one_block, jnp.arange(TOKENS // block_rows, dtype=jnp.int32))
    attended = lax.map(one_head, (query_heads, key_heads, value_heads, lambdas))
    attended = jnp.transpose(attended.reshape(HEADS, TOKENS, DV), (1, 0, 2)).reshape(TOKENS, HEADS * DV)
    projected = jnp.dot(attended, out_weight, preferred_element_type=jnp.float32).astype(jnp.bfloat16)
    resid = (tokens.astype(jnp.float32) + projected.astype(jnp.float32)).astype(jnp.bfloat16)
    resid_full = resid.astype(jnp.float32)
    normed = (resid_full * lax.rsqrt(lax.optimization_barrier(jnp.mean(resid_full * resid_full, axis=1, keepdims=True)) + 1e-06) * mixer_gain).astype(jnp.bfloat16)
    hidden = jnp.square(jax.nn.relu(jnp.dot(normed, up_weight, preferred_element_type=jnp.float32))).astype(jnp.bfloat16)
    return (resid_full + jnp.dot(hidden, down_weight, preferred_element_type=jnp.float32)).astype(jnp.bfloat16)
```

```python
import functools

import jax
import jax.numpy as jnp
from jax import lax
from jax.experimental import pallas as pl
from jax.experimental.pallas import tpu as pltpu
from jax.sharding import Mesh, PartitionSpec as P


DQK = 64
DV = 128
HALF = 512
TILE = 256
BF16 = jnp.bfloat16
F32 = jnp.float32
NEG = -1e30
SEQ = ("z", "y", "c")


ROWS = DV + 16


def attend_kernel(spans, edge, last, ids_ref, lam_ref, q_ref, gain_ref, *refs):
    first = edge == "own"
    if not first:
        top_in, acc_in, *refs = refs
    pieces, refs = refs[: len(spans)], refs[len(spans) :]
    if last:
        out_ref, tops, acc, *refs = refs
    else:
        tops, acc, *refs = refs
    held, sems, items, scores_a, scores_b, peaks_a, peaks_b = refs
    own = ids_ref[0]
    slots = held.shape[0]
    for piece, (slot, half) in zip(pieces, spans):
        target = held.at[slot] if half is None else held.at[slot, pl.ds(half, 1)]
        pltpu.make_async_copy(piece, target, sems.at[slot]).start()
    if first:
        tops[...] = jnp.full(tops.shape, NEG, F32)
        acc[...] = jnp.zeros(acc.shape, F32)
    else:
        tops[...] = top_in[...]
        acc[...] = acc_in[...]

    for slot in range(slots):
        pltpu.make_async_copy(held.at[slot], held.at[slot], sems.at[slot]).wait()

    units = [(t, m) for t in range(HALF // TILE) for m in range(2)]
    parts = 2 * HALF // TILE
    ones = jnp.ones((ROWS - DV, TILE), BF16)

    def columns(side, t):
        return pl.ds(pl.multiple_of(side * HALF, HALF) + t * TILE, TILE)

    def key_part(slot, j):
        return held[slot, j // 2, 2 * (j % 2) : 2 * (j % 2) + 2].reshape(TILE, DV)

    def value_part(slot, j):
        n = 4 + 2 * (j % 2)
        vals = jnp.concatenate([held[slot, j // 2, n], held[slot, j // 2, n + 1]], axis=1)
        return jnp.concatenate([vals, ones], axis=0)

    def score_steps(item, scores, peaks):
        slot, side = item // 2, item % 2
        for u, (t, m) in enumerate(units):
            peak = None
            for j in range(parts):
                s = jnp.dot(
                    key_part(slot, j), q_ref[m, :, columns(side, t)], preferred_element_type=F32
                )
                scores[u, j * TILE : (j + 1) * TILE, :] = s
                high = jnp.max(s.reshape(TILE // 8, 8, TILE), axis=0)
                peak = high if peak is None else jnp.maximum(peak, high)
                if j == parts - 1:
                    peaks[u] = peak
                yield

    def weight_steps(item, scores, peaks):
        slot, side = item // 2, item % 2
        for u, (t, m) in enumerate(units):
            cols = columns(side, t)
            old = tops[m, 0:1, cols]
            top = jnp.maximum(old, jnp.max(peaks[u], axis=0, keepdims=True))
            shrink = jnp.exp(old - top)
            tops[m, 0:1, cols] = top
            total = None
            for j in range(parts):
                p = jnp.exp(scores[u, j * TILE : (j + 1) * TILE, :] - top).astype(BF16)
                part = jnp.dot(value_part(slot, j), p, preferred_element_type=F32)
                total = part if total is None else total + part
                if j == parts - 1:
                    acc[m, :, cols] = acc[m, :, cols] * shrink + total
                yield

    def together(*steps):
        steps = list(steps)
        while steps:
            steps = [s for s in steps if next(s, True) is None]

    def listed(i, count):
        for side, limit in ((0, own), (1, 15 - own)):
            items[count] = 2 * i + side
            count = count + (ids_ref[1 + i] < limit).astype(jnp.int32)
        return count

    def pair(k, carry):
        one, two, three = items[2 * k], items[2 * k + 1], items[2 * k + 2]
        together(score_steps(two, scores_b, peaks_b), weight_steps(one, scores_a, peaks_a))

        @pl.when(2 * k + 1 < count)
        def _():
            together(score_steps(three, scores_a, peaks_a), weight_steps(two, scores_b, peaks_b))

        return carry

    if not first:
        count = lax.fori_loop(0, slots, listed, jnp.int32(0))
        items[count] = 0
        items[count + 1] = 0

        @pl.when(count > 0)
        def _():
            together(score_steps(items[0], scores_a, peaks_a))

        lax.fori_loop(0, (count + 1) // 2, pair, 0)

    def edge_item(slot, side, allowed):
        def tile(t, carry):
            cols = pl.ds(pl.multiple_of(side * HALF + t * TILE, TILE), TILE)
            for m in range(2):
                for j in range(parts):
                    s = jnp.dot(key_part(slot, j), q_ref[m, :, cols], preferred_element_type=F32)
                    key_pos = lax.broadcasted_iota(jnp.int32, (TILE, TILE), 0) + j * TILE
                    query_pos = lax.broadcasted_iota(jnp.int32, (TILE, TILE), 1)
                    scores_a[m, j * TILE : (j + 1) * TILE, :] = jnp.where(
                        key_pos <= query_pos + (t * TILE + allowed), s, -jnp.inf
                    )
            for m in range(2):
                old = tops[m, 0:1, cols]
                top = jnp.maximum(old, jnp.max(scores_a[m], axis=0, keepdims=True))
                shrink = jnp.exp(old - top)
                tops[m, 0:1, cols] = top
                total = None
                for j in range(parts):
                    p = jnp.exp(scores_a[m, j * TILE : (j + 1) * TILE, :] - top).astype(BF16)
                    part = jnp.dot(value_part(slot, j), p, preferred_element_type=F32)
                    total = part if total is None else total + part
                acc[m, :, cols] = acc[m, :, cols] * shrink + total
            return carry

        lax.fori_loop(0, HALF // TILE, tile, 0)

    if edge == "own":
        edge_item(0, 0, 0)

        @pl.when(own < 15 - own)
        def _():
            edge_item(0, 1, 2 * HALF)

    if edge == "other":

        def edges(i, carry):
            @pl.when(ids_ref[1 + i] == 15 - own)
            def _():
                edge_item(i, 1, HALF)

            return carry

        lax.fori_loop(0, slots, edges, 0)

    if last:
        for t in range(2 * HALF // TILE):
            cols = slice(t * TILE, (t + 1) * TILE)
            differ = acc[0, :DV, cols] / acc[0, DV : DV + 1, cols] - lam_ref[0] * (
                acc[1, :DV, cols] / acc[1, DV : DV + 1, cols]
            )
            spread = lax.rsqrt(jnp.mean(differ * differ, axis=0, keepdims=True) + 1e-06)
            out_ref[cols, :] = (differ * spread * gain_ref[...]).T.astype(BF16)


def attend(slots, ids, lam, query, gain, state, edge, last):
    pieces, spans = [], []
    for slot, parts in enumerate(slots):
        if isinstance(parts, tuple):
            for half, part in enumerate(parts):
                pieces.append(part)
                spans.append((slot, half))
        else:
            pieces.append(parts)
            spans.append((slot, None))
    count = len(slots)
    vmem = pl.BlockSpec(memory_space=pltpu.VMEM)
    smem = pl.BlockSpec(memory_space=pltpu.SMEM)
    held = [
        pltpu.VMEM((count, 2, 8, DV, DV), BF16),
        pltpu.SemaphoreType.DMA((count,)),
        pltpu.SMEM((2 * count + 2,), jnp.int32),
        pltpu.VMEM((4, 2 * HALF, TILE), F32),
        pltpu.VMEM((4, 2 * HALF, TILE), F32),
        pltpu.VMEM((4, 8, TILE), F32),
        pltpu.VMEM((4, 8, TILE), F32),
    ]
    shapes = [(2, 8, 2 * HALF), (2, ROWS, 2 * HALF)]
    if last:
        out_shape = jax.ShapeDtypeStruct((2 * HALF, DV), BF16)
        scratch = [pltpu.VMEM(s, F32) for s in shapes] + held
        out_specs = vmem
    else:
        out_shape = tuple(jax.ShapeDtypeStruct(s, F32) for s in shapes)
        scratch = held
        out_specs = (vmem, vmem)
    state = [] if state is None else list(state)
    flops = count * 2 * HALF * HALF * 2 * 2 * 2 * (DV + DV) // 2
    return pl.pallas_call(
        functools.partial(attend_kernel, tuple(spans), edge, last),
        out_shape=out_shape,
        in_specs=[smem, smem, vmem, vmem]
        + [vmem] * len(state)
        + [pl.BlockSpec(memory_space=pl.ANY)] * len(pieces),
        out_specs=out_specs,
        scratch_shapes=scratch,
        cost_estimate=pl.CostEstimate(
            flops=flops, bytes_accessed=count * 2**19, transcendentals=count * 2**20
        ),
        name="attend",
    )(ids, lam, query, gain, *state, *pieces)


def square_relu(x):
    x = jnp.maximum(x, 0.0)
    return (x * x).astype(BF16)


def hidden_units(rows, up, down, copies):
    width = up.shape[2]
    copies[0].wait()
    made = [
        square_relu(
            jnp.dot(
                rows,
                up[:, :, n : n + 512].reshape(-1, 512),
                preferred_element_type=F32,
            )
        )
        for n in range(0, width, 512)
    ]
    made = jnp.concatenate(made, axis=1)
    copies[1].wait()
    return made, down


def down_product(made, down, n):
    return lax.dot_general(
        made,
        down[n // 64 : n // 64 + 8].reshape(512, -1),
        (((1,), (1,)), ((), ())),
        preferred_element_type=F32,
    )


def weight_copies(weight_ref, up, down, sems):
    copies = [
        pltpu.make_async_copy(weight_ref.at[:, 0], up, sems.at[0]),
        pltpu.make_async_copy(weight_ref.at[:, 1], down, sems.at[1]),
    ]
    for copy in copies:
        copy.start()
    return copies


def project_kernel(
    x_ref,
    own_ref,
    prev_ref,
    next_ref,
    far_top_ref,
    far_low_ref,
    proj_ref,
    tokens_ref,
    gain_ref,
    weight_ref,
    resid_ref,
    normed_ref,
    part_ref,
    heads,
    up,
    down,
    sems,
):
    copies = weight_copies(weight_ref, up, down, sems)

    def place(step):
        return pl.ds(pl.multiple_of((x_ref[0] + step) % 4 * 256, 256), 256)

    def group(step):
        return pl.ds(pl.multiple_of((x_ref[0] + step) % 4 * 128, 128), 128)

    heads[:, place(0)] = own_ref[...]
    heads[:, place(3)] = prev_ref[...]
    heads[:, place(1)] = next_ref[...]
    heads[:256, place(2)] = far_top_ref[...]
    heads[256:, place(2)] = far_low_ref[...]
    for r in range(0, 512, 256):
        rows = slice(r, r + 256)
        projected = jnp.dot(heads[rows, :], proj_ref[...], preferred_element_type=F32)
        resid = (tokens_ref[rows, :].astype(F32) + projected.astype(BF16).astype(F32)).astype(BF16)
        heads_wide = resid.astype(F32)
        spread = lax.rsqrt(jnp.mean(heads_wide * heads_wide, axis=1, keepdims=True) + 1e-06)
        normed_ref[rows, :] = (heads_wide * spread * gain_ref[...]).astype(BF16)
        resid_ref[rows, :] = resid
    made, down = hidden_units(normed_ref[group(2), :], up, down, copies)
    for n in range(0, 2048, 512):
        part_ref[:, n : n + 512] = down_product(made, down, n).astype(BF16)


def sides_kernel(x_ref, normed_ref, weight_ref, prev_ref, next_ref, up, down, sems):
    copies = weight_copies(weight_ref, up, down, sems)

    def group(step):
        return pl.ds(pl.multiple_of((x_ref[0] + step) % 4 * 128, 128), 128)

    rows = jnp.concatenate([normed_ref[group(3), :], normed_ref[group(1), :]], axis=0)
    made, down = hidden_units(rows, up, down, copies)
    for n in range(0, 2048, 512):
        part = down_product(made, down, n).astype(BF16)
        prev_ref[:, n : n + 512] = part[:128]
        next_ref[:, n : n + 512] = part[128:]


def own_kernel(x_ref, normed_ref, resid_ref, weight_ref, out_ref, up, down, sems):
    copies = weight_copies(weight_ref, up, down, sems)
    group = pl.ds(pl.multiple_of(x_ref[0] * 128, 128), 128)
    made, down = hidden_units(normed_ref[group, :], up, down, copies)
    for n in range(0, 2048, 512):
        cols = slice(n, n + 512)
        out_ref[:, cols] = down_product(made, down, n) + resid_ref[group, cols].astype(F32)


def feed(kernel, operands, outs, flops, extra=()):
    vmem = pl.BlockSpec(memory_space=pltpu.VMEM)
    return pl.pallas_call(
        kernel,
        out_shape=outs,
        in_specs=[pl.BlockSpec(memory_space=pltpu.SMEM)]
        + [vmem] * (len(operands) - 2)
        + [pl.BlockSpec(memory_space=pl.ANY)],
        out_specs=jax.tree.map(lambda _: vmem, outs),
        scratch_shapes=[
            *extra,
            pltpu.VMEM((32, 64, 1024), BF16),
            pltpu.VMEM((32, 64, 1024), BF16),
            pltpu.SemaphoreType.DMA((2,)),
        ],
        cost_estimate=pl.CostEstimate(flops=flops, bytes_accessed=2**23, transcendentals=0),
    )(*operands)


def ring_pairs(axis, step):
    pairs = []
    for z in range(4):
        for y in range(4):
            for core in range(2):
                if (axis == 1) == (core == 0):
                    to = z * 4 + (y + step) % 4
                else:
                    to = (z + step) % 4 * 4 + y
                pairs.append(((z * 4 + y) * 2 + core, to * 2 + core))
    return pairs


PAIRS = {(axis, step): ring_pairs(axis, step) for axis in (1, 2) for step in (1, -1)}


def passed(array, axis, step):
    return lax.ppermute(array, SEQ, PAIRS[axis, step])


def source_chip(a, b):
    z, y = lax.axis_index("z"), lax.axis_index("y")
    first = lax.axis_index("c") == 0
    dz, dy = jnp.where(first, b, a), jnp.where(first, a, b)
    return (z + dz + 4) % 4 * 4 + (y + dy + 4) % 4


def per_device(
    tokens,
    queries,
    keys,
    values,
    lambdas,
    head_gain,
    out_weight,
    mixer_gain,
    up_weight,
    down_weight,
):
    core = lax.axis_index("c")
    chip = lax.axis_index("z") * 4 + lax.axis_index("y")
    first = core == 0
    swap = [(0, 1), (1, 0)]

    weights = lax.all_gather(jnp.stack([up_weight, down_weight.T]), SEQ, axis=0)
    tokens_all = lax.all_gather(tokens, "x", axis=0, tiled=True)

    def packed(head):
        k = keys[:, head * DV : (head + 1) * DV].reshape(4, DV, DV)
        v = values[:, head * DV : (head + 1) * DV].reshape(4, DV, DV)
        return jnp.concatenate([k, jnp.swapaxes(v, 1, 2)], axis=0)

    head_a, head_b = packed(0), packed(1)
    keep = jnp.where(first, head_a, head_b)
    other = lax.ppermute(jnp.where(first, head_b, head_a), "c", swap)
    chunk = jnp.stack([jnp.where(first, keep, other), jnp.where(first, other, keep)])

    def flat(chip_id, core_id):
        return chip_id * 2 + core_id

    scaled = queries * jnp.asarray(DQK ** (-0.5), BF16)
    query_a, query_b = scaled[:, :DV], scaled[:, DV:]
    over = [(flat(i, 0), flat(i, 1)) for i in range(16)] + [
        (flat(i, 1), flat(15 - i, 0)) for i in range(16)
    ]
    flip = [(flat(i, 1), flat(15 - i, 1)) for i in range(16)]
    got = lax.ppermute(jnp.where(first, query_b, query_a), SEQ, over)
    got_far = lax.ppermute(query_b, SEQ, flip)
    query = jnp.concatenate(
        [jnp.where(first, query_a, got), jnp.where(first, got, got_far)], axis=0
    ).T
    none = jnp.zeros((DQK, 2 * HALF), BF16)
    query = jnp.stack(
        [
            jnp.concatenate([query[:DQK], none], axis=0),
            jnp.concatenate([none, query[DQK:]], axis=0),
        ]
    )

    lam = jnp.where(first, lambdas[0:1], lambdas[1:2])
    gain = head_gain[:, None]

    def attending(slots, state, edge=None, last=False):
        ids = jnp.stack([chip] + [source_chip(*place) for place, _ in slots])
        return attend([c for _, c in slots], ids, lam, query, gain, state, edge, last)

    near_p, near_n = passed(chunk, 1, 1), passed(chunk, 1, -1)
    side_p, side_n = passed(chunk, 2, 1), passed(chunk, 2, -1)
    state = attending([((0, 0), chunk)], None, "own")
    far = passed(near_p[:1], 1, 1), passed(near_n[1:], 1, -1)
    side_pp, side_nn = passed(near_p, 2, 1), passed(near_n, 2, -1)
    side_pn, side_np = passed(near_n, 2, 1), passed(near_p, 2, -1)
    over_0 = passed(side_p, 2, 1)
    state = attending(
        [((-1, 0), near_p), ((1, 0), near_n), ((0, -1), side_p), ((0, 1), side_n)], state
    )
    side_pf = tuple(passed(h, 2, 1) for h in far)
    side_nf = tuple(passed(h, 2, -1) for h in far)
    over_p, over_n = passed(side_pp, 2, 1), passed(side_nn, 2, -1)
    state = attending([((2, 0), far), ((-1, -1), side_pp), ((1, 1), side_nn)], state, "other")
    over_f = tuple(passed(h, 2, -1) for h in side_nf)
    state = attending([((1, -1), side_pn), ((-1, 1), side_np), ((0, 2), over_0)], state, "other")
    rows = attending(
        [((2, -1), side_pf), ((2, 1), side_nf), ((-1, 2), over_p), ((1, 2), over_n), ((2, 2), over_f)],
        state,
        last=True,
    )

    low, high = rows[:HALF], rows[HALF:]
    back = [(flat(i, 1), flat(i, 0)) for i in range(16)] + [
        (flat(i, 0), flat(15 - i, 1)) for i in range(16)
    ]
    got = lax.ppermute(jnp.where(first, high, low), SEQ, back)
    got_far = lax.ppermute(high, SEQ, flip)
    attended = jnp.concatenate(
        [jnp.where(first, low, got), jnp.where(first, got, got_far)], axis=1
    )


    def along_x(array, step):
        return lax.ppermute(array, "x", [(i, (i + step) % 4) for i in range(4)])

    prev, following = along_x(attended, 1), along_x(attended, -1)
    far_top = along_x(prev[:256], 1)
    far_low = along_x(following[256:], -1)
    x = lax.axis_index("x")[None]
    part = jax.ShapeDtypeStruct((128, 2048), BF16)
    wide = jax.ShapeDtypeStruct((512, 2048), BF16)
    one = 2 * 2 * 128 * 2048 * 1024
    resid, normed, far_part = feed(
        project_kernel,
        (
            x,
            attended,
            prev,
            following,
            far_top,
            far_low,
            out_weight,
            tokens_all,
            mixer_gain[None],
            weights,
        ),
        (wide, wide, part),
        2 * one,
        (pltpu.VMEM((512, 1024), BF16),),
    )
    from_prev = along_x(far_part[:64], 1)
    from_next = along_x(far_part[64:], -1)
    prev_part, next_part = feed(sides_kernel, (x, normed, weights), (part, part), 2 * one)

    def added(a, b):
        return (a.astype(F32) + b.astype(F32)).astype(BF16)

    to_next = jnp.concatenate([added(next_part[:64], from_prev), next_part[64:]], axis=0)
    to_prev = jnp.concatenate([prev_part[:64], added(prev_part[64:], from_next)], axis=0)
    got_prev = along_x(to_next, 1)
    got_next = along_x(to_prev, -1)
    total = feed(
        own_kernel, (x, normed, resid, weights), jax.ShapeDtypeStruct((128, 2048), F32), one
    )
    return (total + got_prev.astype(F32) + got_next.astype(F32)).astype(BF16)


def solution(mesh):
    grid = Mesh(mesh.devices.reshape(4, 4, 2, 4), ("z", "y", "c", "x"))
    placed = (
        P((*SEQ, "x"), None),
        P(SEQ, "x"),
        P(SEQ, "x"),
        P(SEQ, "x"),
        P("x"),
        P(),
        P(),
        P(),
        P(SEQ, "x"),
        P("x", SEQ),
    )

    return jax.shard_map(
        per_device, mesh=grid, in_specs=placed, out_specs=P((*SEQ, "x"), None), check_vma=False
    )
```

```python
import functools

import jax
import jax.numpy as jnp
from jax import lax
from jax.experimental import pallas as pl
from jax.experimental.pallas import tpu as pltpu
from jax.sharding import Mesh, PartitionSpec as P


DQK = 64
DV = 128
HALF = 512
TILE = 256
BF16 = jnp.bfloat16
F32 = jnp.float32
NEG = -1e30
SEQ = ("z", "y", "c")


ROWS = DV + 16


def attend_kernel(spans, edge, last, ids_ref, lam_ref, q_ref, gain_ref, *refs):
    first = edge == "own"
    if not first:
        top_in, acc_in, *refs = refs
    pieces, refs = refs[: len(spans)], refs[len(spans) :]
    if last:
        low_ref, high_ref, tops, acc, *refs = refs
    else:
        tops, acc, *refs = refs
    held, sems, items, scores_a, scores_b, peaks_a, peaks_b = refs
    own = ids_ref[0]
    slots = held.shape[0]
    slot = 0
    for piece, span in zip(pieces, spans):
        for j in range(span):
            pltpu.make_async_copy(piece.at[j], held.at[slot], sems.at[slot]).start()
            slot += 1
    if first:
        tops[...] = jnp.full(tops.shape, NEG, F32)
        acc[...] = jnp.zeros(acc.shape, F32)
    else:
        tops[...] = top_in[...]
        acc[...] = acc_in[...]

    for slot in range(slots):
        pltpu.make_async_copy(held.at[slot], held.at[slot], sems.at[slot]).wait()

    units = [(t, m) for t in range(HALF // TILE) for m in range(2)]
    parts = 2 * HALF // TILE
    ones = jnp.ones((ROWS - DV, TILE), BF16)

    def columns(side, t):
        return pl.ds(pl.multiple_of(side * HALF, HALF) + t * TILE, TILE)

    def key_part(slot, j):
        return held[slot, j // 2, 2 * (j % 2) : 2 * (j % 2) + 2].reshape(TILE, DV)

    def value_part(slot, j):
        n = 4 + 2 * (j % 2)
        vals = jnp.concatenate([held[slot, j // 2, n], held[slot, j // 2, n + 1]], axis=1)
        return jnp.concatenate([vals, ones], axis=0)

    def score_steps(item, scores, peaks):
        slot, side = item // 2, item % 2
        for u, (t, m) in enumerate(units):
            peak = None
            for j in range(parts):
                s = jnp.dot(
                    key_part(slot, j), q_ref[m, :, columns(side, t)], preferred_element_type=F32
                )
                scores[u, j * TILE : (j + 1) * TILE, :] = s
                high = jnp.max(s.reshape(TILE // 8, 8, TILE), axis=0)
                peak = high if peak is None else jnp.maximum(peak, high)
                if j == parts - 1:
                    peaks[u] = peak
                yield

    def weight_steps(item, scores, peaks):
        slot, side = item // 2, item % 2
        for u, (t, m) in enumerate(units):
            cols = columns(side, t)
            old = tops[m, 0:1, cols]
            top = jnp.maximum(old, jnp.max(peaks[u], axis=0, keepdims=True))
            shrink = jnp.exp(old - top)
            tops[m, 0:1, cols] = top
            total = None
            for j in range(parts):
                p = jnp.exp(scores[u, j * TILE : (j + 1) * TILE, :] - top).astype(BF16)
                part = jnp.dot(value_part(slot, j), p, preferred_element_type=F32)
                total = part if total is None else total + part
                if j == parts - 1:
                    acc[m, :, cols] = acc[m, :, cols] * shrink + total
                yield

    def together(*steps):
        steps = list(steps)
        while steps:
            steps = [s for s in steps if next(s, True) is None]

    def listed(i, count):
        for side, limit in ((0, own), (1, 15 - own)):
            items[count] = 2 * i + side
            count = count + (ids_ref[1 + i] < limit).astype(jnp.int32)
        return count

    def pair(k, carry):
        one, two, three = items[2 * k], items[2 * k + 1], items[2 * k + 2]
        together(score_steps(two, scores_b, peaks_b), weight_steps(one, scores_a, peaks_a))

        @pl.when(2 * k + 1 < count)
        def _():
            together(score_steps(three, scores_a, peaks_a), weight_steps(two, scores_b, peaks_b))

        return carry

    if not first:
        count = lax.fori_loop(0, slots, listed, jnp.int32(0))
        items[count] = 0
        items[count + 1] = 0

        @pl.when(count > 0)
        def _():
            together(score_steps(items[0], scores_a, peaks_a))

        lax.fori_loop(0, (count + 1) // 2, pair, 0)

    def edge_item(slot, side, allowed):
        def tile(t, carry):
            cols = pl.ds(pl.multiple_of(side * HALF + t * TILE, TILE), TILE)
            for m in range(2):
                for j in range(parts):
                    s = jnp.dot(key_part(slot, j), q_ref[m, :, cols], preferred_element_type=F32)
                    key_pos = lax.broadcasted_iota(jnp.int32, (TILE, TILE), 0) + j * TILE
                    query_pos = lax.broadcasted_iota(jnp.int32, (TILE, TILE), 1)
                    scores_a[m, j * TILE : (j + 1) * TILE, :] = jnp.where(
                        key_pos <= query_pos + (t * TILE + allowed), s, -jnp.inf
                    )
            for m in range(2):
                old = tops[m, 0:1, cols]
                top = jnp.maximum(old, jnp.max(scores_a[m], axis=0, keepdims=True))
                shrink = jnp.exp(old - top)
                tops[m, 0:1, cols] = top
                total = None
                for j in range(parts):
                    p = jnp.exp(scores_a[m, j * TILE : (j + 1) * TILE, :] - top).astype(BF16)
                    part = jnp.dot(value_part(slot, j), p, preferred_element_type=F32)
                    total = part if total is None else total + part
                acc[m, :, cols] = acc[m, :, cols] * shrink + total
            return carry

        lax.fori_loop(0, HALF // TILE, tile, 0)

    if edge == "own":
        edge_item(0, 0, 0)

        @pl.when(own < 15 - own)
        def _():
            edge_item(0, 1, 2 * HALF)

    if edge == "other":

        def edges(i, carry):
            @pl.when(ids_ref[1 + i] == 15 - own)
            def _():
                edge_item(i, 1, HALF)

            return carry

        lax.fori_loop(0, slots, edges, 0)

    if last:
        for t in range(2 * HALF // TILE):
            cols = slice(t * TILE, (t + 1) * TILE)
            differ = acc[0, :DV, cols] / acc[0, DV : DV + 1, cols] - lam_ref[0] * (
                acc[1, :DV, cols] / acc[1, DV : DV + 1, cols]
            )
            spread = lax.rsqrt(jnp.mean(differ * differ, axis=0, keepdims=True) + 1e-06)
            out_ref = low_ref if t * TILE < HALF else high_ref
            rows = slice(t * TILE % HALF, t * TILE % HALF + TILE)
            out_ref[rows, :] = (differ * spread * gain_ref[...]).T.astype(BF16)


def attend(slots, ids, lam, query, gain, state, edge, last):
    pieces = [p if p.ndim == 5 else p[None] for p in slots]
    spans = tuple(p.shape[0] for p in pieces)
    count = sum(spans)
    vmem = pl.BlockSpec(memory_space=pltpu.VMEM)
    smem = pl.BlockSpec(memory_space=pltpu.SMEM)
    held = [
        pltpu.VMEM((count, 2, 8, DV, DV), BF16),
        pltpu.SemaphoreType.DMA((count,)),
        pltpu.SMEM((2 * count + 2,), jnp.int32),
        pltpu.VMEM((4, 2 * HALF, TILE), F32),
        pltpu.VMEM((4, 2 * HALF, TILE), F32),
        pltpu.VMEM((4, 8, TILE), F32),
        pltpu.VMEM((4, 8, TILE), F32),
    ]
    shapes = [(2, 8, 2 * HALF), (2, ROWS, 2 * HALF)]
    if last:
        out_shape = (jax.ShapeDtypeStruct((HALF, DV), BF16),) * 2
        scratch = [pltpu.VMEM(s, F32) for s in shapes] + held
        out_specs = (vmem, vmem)
    else:
        out_shape = tuple(jax.ShapeDtypeStruct(s, F32) for s in shapes)
        scratch = held
        out_specs = (vmem, vmem)
    state = [] if state is None else list(state)
    flops = count * 2 * HALF * HALF * 2 * 2 * 2 * (DV + DV) // 2
    return pl.pallas_call(
        functools.partial(attend_kernel, spans, edge, last),
        out_shape=out_shape,
        in_specs=[smem, smem, vmem, vmem]
        + [vmem] * len(state)
        + [pl.BlockSpec(memory_space=pl.ANY)] * len(pieces),
        out_specs=out_specs,
        scratch_shapes=scratch,
        cost_estimate=pl.CostEstimate(
            flops=flops, bytes_accessed=count * 2**19, transcendentals=count * 2**20
        ),
        name="attend",
    )(ids, lam, query, gain, *state, *pieces)


def square_relu(x):
    x = jnp.maximum(x, 0.0)
    return (x * x).astype(BF16)


CUTS = 8


def token_kernel(steps, x_ref, chips_ref, gain_ref, *refs):
    tokens_refs, refs = refs[: len(steps)], refs[len(steps) :]
    heads_refs, proj_ref, refs = refs[:5], refs[5], refs[6:]
    weight_refs, refs = refs[:10], refs[10:]
    outs, (heads, tokens, proj, up, down, sems) = refs[:-6], refs[-6:]
    x = x_ref[0]

    def copied(source, target, n):
        pltpu.make_async_copy(source, target, sems.at[n]).start()

    def settled(target, n):
        pltpu.make_async_copy(target, target, sems.at[n]).wait()

    for g, step in enumerate(steps):
        who = (x + step) % 4
        rows = pl.ds(pl.multiple_of(who * 128, 128), 128)
        here = pl.ds(g * 128, 128)
        copied(tokens_refs[g], tokens.at[here], 1)
        for back, source in zip((0, 3, 1), heads_refs):
            cols = pl.ds(pl.multiple_of((x + back) % 4 * 256, 256), 256)
            copied(source.at[rows], heads.at[here, cols], 0)
        cols = pl.ds(pl.multiple_of((x + 2) % 4 * 256, 256), 256)
        half = pl.ds(pl.multiple_of(who % 2 * 128, 128), 128)

        @pl.when(who < 2)
        def _(half=half, here=here, cols=cols):
            copied(heads_refs[3].at[half], heads.at[here, cols], 0)

        @pl.when(who >= 2)
        def _(half=half, here=here, cols=cols):
            copied(heads_refs[4].at[half], heads.at[here, cols], 0)

    for n in range(CUTS):
        part = pl.ds(n * 1024 // CUTS, 1024 // CUTS)
        copied(proj_ref.at[part], proj.at[part], 2)
    for kind, target in enumerate((up, down)):
        for half in range(2):
            slot = 0
            for piece in weight_refs[5 * half : 5 * half + 5]:
                for j in range(piece.shape[0]):
                    copied(
                        piece.at[j, kind], target.at[half, chips_ref[16 * half + slot]], 3 + kind
                    )
                    slot += 1

    settled(heads, 0)
    settled(tokens, 1)
    settled(proj, 2)
    projected = jnp.dot(heads[...], proj[...], preferred_element_type=F32).astype(BF16)
    resid = (tokens[...].astype(F32) + projected.astype(F32)).astype(BF16)
    wide = resid.astype(F32)
    spread = lax.rsqrt(jnp.mean(wide * wide, axis=1, keepdims=True) + 1e-06)
    tokens[...] = resid
    normed = (wide * spread * gain_ref[...]).astype(BF16)
    settled(up, 3)
    made = [
        square_relu(
            jnp.dot(normed, up[half].reshape(2048, 512), preferred_element_type=F32)
        )
        for half in range(2)
    ]
    settled(down, 4)
    for n in range(0, 2048, 512):
        cols = slice(n, n + 512)
        part = None
        for half in range(2):
            term = lax.dot_general(
                made[half],
                down[half, n // 128 : n // 128 + 4].reshape(512, 512),
                (((1,), (1,)), ((), ())),
                preferred_element_type=F32,
            )
            part = term if part is None else part + term
        if steps == (0,):
            outs[0][:, cols] = part + tokens[:, cols].astype(F32)
        else:
            size = outs[0].shape[0]
            for g, out in enumerate(outs):
                out[:, cols] = part[g * size : (g + 1) * size].astype(BF16)


def token_parts(steps, x, chips, gain, tokens, parts):
    count = len(steps)
    pieces = 1 if steps == (0,) else 2
    kind = F32 if steps == (0,) else BF16
    vmem = pl.BlockSpec(memory_space=pltpu.VMEM)
    smem = pl.BlockSpec(memory_space=pltpu.SMEM)
    return pl.pallas_call(
        functools.partial(token_kernel, steps),
        out_shape=[jax.ShapeDtypeStruct((count * 128 // pieces, 2048), kind)] * pieces,
        in_specs=[smem, smem, vmem]
        + [pl.BlockSpec(memory_space=pl.ANY)] * (count + len(parts)),
        out_specs=[vmem] * pieces,
        scratch_shapes=[
            pltpu.VMEM((count * 128, 1024), BF16),
            pltpu.VMEM((count * 128, 2048), BF16),
            pltpu.VMEM((1024, 2048), BF16),
            pltpu.VMEM((2, 16, 128, 512), BF16),
            pltpu.VMEM((2, 16, 128, 512), BF16),
            pltpu.SemaphoreType.DMA((5,)),
        ],
        cost_estimate=pl.CostEstimate(
            flops=count * 128 * 2048 * 3072 * 2, bytes_accessed=12 * 2**20, transcendentals=0
        ),
        name="token_parts",
    )(x, chips, gain, *tokens, *parts)


def ring_pairs(axis, step):
    pairs = []
    for z in range(4):
        for y in range(4):
            for core in range(2):
                if (axis == 1) == (core == 0):
                    to = z * 4 + (y + step) % 4
                else:
                    to = (z + step) % 4 * 4 + y
                pairs.append(((z * 4 + y) * 2 + core, to * 2 + core))
    return pairs


PAIRS = {(axis, step): ring_pairs(axis, step) for axis in (1, 2) for step in (1, -1)}


def passed(array, axis, step):
    return lax.ppermute(array, SEQ, PAIRS[axis, step])


def source_chip(a, b, core=0):
    z, y = lax.axis_index("z"), lax.axis_index("y")
    first = lax.axis_index("c") == core
    dz, dy = jnp.where(first, b, a), jnp.where(first, a, b)
    return (z + dz + 4) % 4 * 4 + (y + dy + 4) % 4


def per_device(
    tokens,
    queries,
    keys,
    values,
    lambdas,
    head_gain,
    out_weight,
    mixer_gain,
    up_weight,
    down_weight,
):
    core = lax.axis_index("c")
    chip = lax.axis_index("z") * 4 + lax.axis_index("y")
    first = core == 0
    swap = [(0, 1), (1, 0)]

    def along_x(array, step):
        return lax.ppermute(array, "x", [(i, (i + step) % 4) for i in range(4)])

    def swapped(array):
        return lax.ppermute(array, "c", swap)

    scaled = queries * jnp.asarray(DQK ** (-0.5), BF16)

    def packed(head):
        cols = slice(head * DV, (head + 1) * DV)
        k = keys[:, cols].reshape(4, DV, DV)
        v = values[:, cols].reshape(4, DV, DV)
        q = scaled[:, cols].reshape(4, DV, DV)
        return jnp.concatenate([k, jnp.swapaxes(v, 1, 2), q], axis=0)

    head_a, head_b = packed(0), packed(1)
    keep = jnp.where(first, head_a, head_b)
    other = swapped(jnp.where(first, head_b, head_a))
    even, odd = jnp.where(first, keep, other), jnp.where(first, other, keep)
    chunk = jnp.stack([even[:8], odd[:8]])

    def flat(chip_id, core_id):
        return chip_id * 2 + core_id

    high = lax.ppermute(odd[8:], ("z", "y"), [(i, 15 - i) for i in range(16)])
    query = jnp.concatenate([even[8:].reshape(HALF, DV), high.reshape(HALF, DV)], axis=0).T
    none = jnp.zeros((DQK, 2 * HALF), BF16)
    query = jnp.stack(
        [
            jnp.concatenate([query[:DQK], none], axis=0),
            jnp.concatenate([none, query[DQK:]], axis=0),
        ]
    )

    lam = jnp.where(first, lambdas[0:1], lambdas[1:2])
    gain = head_gain[:, None]

    def attending(slots, state, edge=None, last=False):
        places = [p for place, _ in slots for p in (place if isinstance(place[0], tuple) else (place,))]
        ids = jnp.stack([chip] + [source_chip(*place) for place in places])
        return attend([c for _, c in slots], ids, lam, query, gain, state, edge, last)

    near_p, near_n = passed(chunk, 1, 1), passed(chunk, 1, -1)
    state = attending([((0, 0), chunk)], None, "own")
    across = passed(near_p, 1, 1)
    pair_a = jnp.stack([chunk, near_p])
    a_p, a_n = passed(pair_a, 2, 1), passed(pair_a, 2, -1)
    pair_b = jnp.stack([near_n, across])
    b_p, b_n = passed(pair_b, 2, 1), passed(pair_b, 2, -1)
    over_p = passed(a_p, 2, 1)
    state = attending(
        [
            ((-1, 0), near_p),
            ((1, 0), near_n),
            ((2, 0), across),
            (((0, -1), (-1, -1)), a_p),
            (((0, 1), (-1, 1)), a_n),
        ],
        state,
        "other",
    )
    over_n = passed(b_n, 2, -1)
    state = attending([(((1, -1), (2, -1)), b_p), (((1, 1), (2, 1)), b_n)], state, "other")

    tokens_p, tokens_n = along_x(tokens, 1), along_x(tokens, -1)
    tokens_far = along_x(tokens_p, 1)
    both = jnp.stack([up_weight, down_weight.T])
    both_a, both_b = both[:, :, :512], both[:, :, 512:]
    keep = jnp.where(first, both_a, both_b)
    other = swapped(jnp.where(first, both_b, both_a))
    unit = jnp.concatenate(
        [jnp.where(first, keep, other), jnp.where(first, other, keep)], axis=1
    )
    unit_p, unit_n = passed(unit, 1, 1), passed(unit, 1, -1)
    unit_f = passed(unit_p, 1, 1)
    row = jnp.stack([unit, unit_p, unit_n, unit_f])
    row_p, row_n = passed(row, 2, 1), passed(row, 2, -1)
    row_a, row_b = passed(row_p[:2], 2, 1), passed(row_n[2:], 2, -1)
    weights = [row, row_p, row_n, row_a, row_b]
    weights += [swapped(w) for w in weights]
    near = (0, -1, 1, 2)
    chips = jnp.stack(
        [
            source_chip(a, b, core)
            for core in (0, 1)
            for places in ((near, 0), (near, -1), (near, 1), (near, 2))
            for a, b in ((n, places[1]) for n in places[0])
        ]
    )
    low, high = attending(
        [(((0, 2), (-1, 2)), over_p), (((1, 2), (2, 2)), over_n)], state, last=True
    )

    back = [(flat(i, 1), flat(i, 0)) for i in range(16)] + [
        (flat(i, 0), flat(15 - i, 1)) for i in range(16)
    ]
    flip = [(flat(i, 1), flat(15 - i, 1)) for i in range(16)]
    got_far = lax.ppermute(high, SEQ, flip)
    got = lax.ppermute(jnp.where(first, high, low), SEQ, back)
    attended = jnp.concatenate([jnp.where(first, low, got), jnp.where(first, got, got_far)], axis=1)

    prev, following = along_x(attended, 1), along_x(attended, -1)
    far_top = along_x(prev[:256], 1)
    far_low = along_x(following[256:], -1)
    x = lax.axis_index("x")[None]
    parts = (attended, prev, following, far_top, far_low, out_weight, *weights)
    gain = mixer_gain[None]
    far_top_part, far_low_part = token_parts((2,), x, chips, gain, (tokens_far,), parts)
    from_prev = along_x(far_top_part, 1)
    from_next = along_x(far_low_part, -1)
    prev_part, next_part = token_parts((3, 1), x, chips, gain, (tokens_p, tokens_n), parts)

    def added(a, b):
        return (a.astype(F32) + b.astype(F32)).astype(BF16)

    none = jnp.zeros((64, 2048), BF16)
    to_next = added(next_part, jnp.concatenate([from_prev, none], axis=0))
    to_prev = added(prev_part, jnp.concatenate([none, from_next], axis=0))
    got_prev = along_x(to_next, 1)
    got_next = along_x(to_prev, -1)
    (total,) = token_parts((0,), x, chips, gain, (tokens,), parts)
    return (total + got_prev.astype(F32) + got_next.astype(F32)).astype(BF16)


def solution(mesh):
    grid = Mesh(mesh.devices.reshape(4, 4, 2, 4), ("z", "y", "c", "x"))
    placed = (
        P((*SEQ, "x"), None),
        P(SEQ, "x"),
        P(SEQ, "x"),
        P(SEQ, "x"),
        P("x"),
        P(),
        P(),
        P(),
        P(SEQ, "x"),
        P("x", SEQ),
    )

    return jax.shard_map(
        per_device, mesh=grid, in_specs=placed, out_specs=P((*SEQ, "x"), None), check_vma=False
    )
```

```python
import functools

import jax
import jax.numpy as jnp
from jax import lax
from jax.experimental import pallas as pl
from jax.experimental.pallas import tpu as pltpu
from jax.sharding import Mesh, PartitionSpec as P


DQK = 64
DV = 128
HALF = 512
TILE = 256
BF16 = jnp.bfloat16
F32 = jnp.float32
NEG = -1e30
SEQ = ("z", "y", "c")


ROWS = DV + 16


def attend_kernel(spans, at, edge, last, ids_ref, lam_ref, q_ref, gain_ref, *refs):
    first = edge == "own"
    if not first:
        top_in, acc_in, *refs = refs
    pieces, refs = refs[: len(spans)], refs[len(spans) :]
    if last:
        low_ref, high_ref, tops, acc, *refs = refs
    else:
        tops, acc, *refs = refs
    held, sems, items, seen, scores_a, scores_b, peaks_a, peaks_b = refs
    own = ids_ref[0]
    slots = held.shape[0]
    slot = 0
    for piece, span in zip(pieces, spans):
        for j in range(span):
            pltpu.make_async_copy(piece.at[j], held.at[slot], sems.at[slot]).start()
            slot += 1
    if first:
        tops[...] = jnp.full(tops.shape, NEG, F32)
        acc[...] = jnp.zeros(acc.shape, F32)
    else:
        tops[...] = top_in[...]
        acc[...] = acc_in[...]

    seen[0] = 0

    units = [(t, m) for t in range(HALF // TILE) for m in range(2)]
    parts = 2 * HALF // TILE
    ones = jnp.ones((ROWS - DV, TILE), BF16)

    def columns(side, t):
        return pl.ds(pl.multiple_of(side * HALF, HALF) + t * TILE, TILE)

    def key_part(slot, j):
        return held[slot, j // 2, 2 * (j % 2) : 2 * (j % 2) + 2].reshape(TILE, DV)

    def value_part(slot, j):
        n = 4 + 2 * (j % 2)
        vals = jnp.concatenate([held[slot, j // 2, n], held[slot, j // 2, n + 1]], axis=1)
        return jnp.concatenate([vals, ones], axis=0)

    def score_steps(item, scores, peaks):
        slot, side = item // 2, item % 2
        for u, (t, m) in enumerate(units):
            peak = None
            for j in range(parts):
                s = jnp.dot(
                    key_part(slot, j), q_ref[m, :, columns(side, t)], preferred_element_type=F32
                )
                scores[u, j * TILE : (j + 1) * TILE, :] = s
                high = jnp.max(s.reshape(TILE // 8, 8, TILE), axis=0)
                peak = high if peak is None else jnp.maximum(peak, high)
                if j == parts - 1:
                    peaks[u] = peak
                yield

    def weight_steps(item, scores, peaks):
        slot, side = item // 2, item % 2
        for u, (t, m) in enumerate(units):
            cols = columns(side, t)
            old = tops[m, 0:1, cols]
            top = jnp.maximum(old, jnp.max(peaks[u], axis=0, keepdims=True))
            shrink = jnp.exp(old - top)
            tops[m, 0:1, cols] = top
            total = None
            for j in range(parts):
                p = jnp.exp(scores[u, j * TILE : (j + 1) * TILE, :] - top).astype(BF16)
                part = jnp.dot(value_part(slot, j), p, preferred_element_type=F32)
                total = part if total is None else total + part
                if j == parts - 1:
                    acc[m, :, cols] = acc[m, :, cols] * shrink + total
                yield

    def together(*steps):
        steps = list(steps)
        while steps:
            steps = [s for s in steps if next(s, True) is None]

    def listed():
        count = jnp.int32(0)
        for i in range(slots):
            for side, limit in ((0, own), (1, 15 - own)):
                items[count] = 2 * i + side
                count = count + (ids_ref[at[i]] < limit).astype(jnp.int32)
        return count

    def ready(item):
        def one(slot, carry):
            pltpu.make_async_copy(held.at[slot], held.at[slot], sems.at[slot]).wait()
            return carry

        lax.fori_loop(seen[0], item // 2 + 1, one, 0)
        seen[0] = jnp.maximum(seen[0], item // 2 + 1)

    def pair(k, carry):
        one, two, three = items[2 * k], items[2 * k + 1], items[2 * k + 2]
        ready(two)
        together(score_steps(two, scores_b, peaks_b), weight_steps(one, scores_a, peaks_a))

        @pl.when(2 * k + 1 < count)
        def _():
            ready(three)
            together(score_steps(three, scores_a, peaks_a), weight_steps(two, scores_b, peaks_b))

        return carry

    if not first:
        count = listed()
        items[count] = 0
        items[count + 1] = 0

        @pl.when(count > 0)
        def _():
            ready(items[0])
            together(score_steps(items[0], scores_a, peaks_a))

        lax.fori_loop(0, (count + 1) // 2, pair, 0)

    def edge_item(slot, side, allowed):
        def tile(t, carry):
            cols = pl.ds(pl.multiple_of(side * HALF + t * TILE, TILE), TILE)
            for m in range(2):
                for j in range(parts):
                    s = jnp.dot(key_part(slot, j), q_ref[m, :, cols], preferred_element_type=F32)
                    key_pos = lax.broadcasted_iota(jnp.int32, (TILE, TILE), 0) + j * TILE
                    query_pos = lax.broadcasted_iota(jnp.int32, (TILE, TILE), 1)
                    scores_a[m, j * TILE : (j + 1) * TILE, :] = jnp.where(
                        key_pos <= query_pos + (t * TILE + allowed), s, -jnp.inf
                    )
            for m in range(2):
                old = tops[m, 0:1, cols]
                top = jnp.maximum(old, jnp.max(scores_a[m], axis=0, keepdims=True))
                shrink = jnp.exp(old - top)
                tops[m, 0:1, cols] = top
                total = None
                for j in range(parts):
                    p = jnp.exp(scores_a[m, j * TILE : (j + 1) * TILE, :] - top).astype(BF16)
                    part = jnp.dot(value_part(slot, j), p, preferred_element_type=F32)
                    total = part if total is None else total + part
                acc[m, :, cols] = acc[m, :, cols] * shrink + total
            return carry

        lax.fori_loop(0, HALF // TILE, tile, 0)

    ready(2 * slots - 2)
    if edge == "own":
        edge_item(0, 0, 0)

        @pl.when(own < 15 - own)
        def _():
            edge_item(0, 1, 2 * HALF)

    if edge == "other":

        here = jnp.int32(-1)
        for i in range(slots):
            here = jnp.where(ids_ref[at[i]] == 15 - own, i, here)

        @pl.when(here >= 0)
        def _():
            edge_item(here, 1, HALF)

    if last:
        for t in range(2 * HALF // TILE):
            cols = slice(t * TILE, (t + 1) * TILE)
            differ = acc[0, :DV, cols] / acc[0, DV : DV + 1, cols] - lam_ref[0] * (
                acc[1, :DV, cols] / acc[1, DV : DV + 1, cols]
            )
            spread = lax.rsqrt(jnp.mean(differ * differ, axis=0, keepdims=True) + 1e-06)
            out_ref = low_ref if t * TILE < HALF else high_ref
            rows = slice(t * TILE % HALF, t * TILE % HALF + TILE)
            out_ref[rows, :] = ((differ * spread).T * gain_ref[...]).astype(BF16)


def attend(slots, at, ids, lam, query, gain, state, edge, last):
    pieces = [p if p.ndim == 5 else p[None] for p in slots]
    spans = tuple(p.shape[0] for p in pieces)
    count = sum(spans)
    vmem = pl.BlockSpec(memory_space=pltpu.VMEM)
    smem = pl.BlockSpec(memory_space=pltpu.SMEM)
    held = [
        pltpu.VMEM((count, 2, 8, DV, DV), BF16),
        pltpu.SemaphoreType.DMA((count,)),
        pltpu.SMEM((2 * count + 2,), jnp.int32),
        pltpu.SMEM((1,), jnp.int32),
        pltpu.VMEM((4, 2 * HALF, TILE), F32),
        pltpu.VMEM((4, 2 * HALF, TILE), F32),
        pltpu.VMEM((4, 8, TILE), F32),
        pltpu.VMEM((4, 8, TILE), F32),
    ]
    shapes = [(2, 8, 2 * HALF), (2, ROWS, 2 * HALF)]
    if last:
        out_shape = (jax.ShapeDtypeStruct((HALF, DV), BF16),) * 2
        scratch = [pltpu.VMEM(s, F32) for s in shapes] + held
        out_specs = (vmem, vmem)
    else:
        out_shape = tuple(jax.ShapeDtypeStruct(s, F32) for s in shapes)
        scratch = held
        out_specs = (vmem, vmem)
    state = [] if state is None else list(state)
    flops = count * 2 * HALF * HALF * 2 * 2 * 2 * (DV + DV) // 2
    return pl.pallas_call(
        functools.partial(attend_kernel, spans, at, edge, last),
        out_shape=out_shape,
        in_specs=[smem, smem, vmem, vmem]
        + [vmem] * len(state)
        + [pl.BlockSpec(memory_space=pl.ANY)] * len(pieces),
        out_specs=out_specs,
        scratch_shapes=scratch,
        cost_estimate=pl.CostEstimate(
            flops=flops, bytes_accessed=count * 2**19, transcendentals=count * 2**20
        ),
        compiler_params=pltpu.CompilerParams(vmem_limit_bytes=26 * 2**20),
        name="attend",
    )(ids, lam, query, gain, *state, *pieces)


def square_relu(x):
    x = jnp.maximum(x, 0.0)
    return (x * x).astype(BF16)


CUTS = 8
EARLY = 3


def token_kernel(steps, x_ref, chips_ref, gain_ref, *refs):
    tokens_refs, refs = refs[: len(steps)], refs[len(steps) :]
    heads_refs, proj_ref, refs = refs[:5], refs[5], refs[6:]
    weight_refs, refs = refs[:10], refs[10:]
    outs, (plain, ordered, total, proj, late, sems) = refs[:-6], refs[-6:]
    x = x_ref[0]
    for n in range(CUTS):
        part = pl.ds(n * 1024 // CUTS, 1024 // CUTS)
        pltpu.make_async_copy(proj_ref.at[part], proj.at[part], sems.at[0]).start()
    slot, held = 0, []
    for piece in weight_refs:
        if len(held) < EARLY:
            held.append(piece)
            continue
        place = pl.ds(slot, piece.shape[0])
        pltpu.make_async_copy(piece, late.at[place], sems.at[1]).start()
        held.append(late.at[place])
        slot += piece.shape[0]

    def lanes(chip):
        return pl.ds(pl.multiple_of(chip * 128, 128), 128)

    def gathered(back):
        found = []
        for step in steps:
            who = (x + step) % 4
            rows = pl.ds(pl.multiple_of(who * 128, 128), 128)
            half = pl.ds(pl.multiple_of(who % 2 * 128, 128), 128)
            if back == 2:
                top, low = heads_refs[3][half, :], heads_refs[4][half, :]
                found.append(jnp.where(who < 2, top, low))
            else:
                found.append(heads_refs[(0, 3, 1).index(back)][rows, :])
        return found[0] if len(found) == 1 else jnp.concatenate(found, axis=0)

    projected = None
    pltpu.make_async_copy(proj, proj, sems.at[0]).wait()
    for back in (0, 3, 1, 2):
        rows = pl.ds(pl.multiple_of((x + back) % 4 * 256, 256), 256)
        term = jnp.dot(gathered(back), proj[rows, :], preferred_element_type=F32)
        projected = term if projected is None else projected + term
    tokens = [t[...] for t in tokens_refs]
    tokens = tokens[0] if len(tokens) == 1 else jnp.concatenate(tokens, axis=0)
    resid = (tokens.astype(F32) + projected.astype(BF16).astype(F32)).astype(BF16)
    wide = resid.astype(F32)
    spread = lax.rsqrt(jnp.mean(wide * wide, axis=1, keepdims=True) + 1e-06)
    plain[...] = (wide * spread * gain_ref[...]).astype(BF16)

    for half in range(2):
        for slot in range(16):
            ordered[half, :, slot * 128 : (slot + 1) * 128] = plain[
                :, lanes(chips_ref[1 + 16 * half + slot])
            ]
    pltpu.make_async_copy(late, late, sems.at[1]).wait()
    for half in range(2):
        pieces = held[5 * half : 5 * half + 5]
        made, at = None, 0
        for piece in pieces:
            depth = piece.shape[0] * 128
            term = jnp.dot(
                ordered[half, :, at : at + depth],
                piece[:, 0].reshape(depth, 512),
                preferred_element_type=F32,
            )
            made = term if made is None else made + term
            at += depth
        made = square_relu(made)
        slot = 0
        for piece in pieces:
            depth = piece.shape[0] * 128
            part = lax.dot_general(
                made,
                piece[:, 1].reshape(depth, 512),
                (((1,), (1,)), ((), ())),
                preferred_element_type=F32,
            )
            for j in range(piece.shape[0]):
                here = lanes(chips_ref[1 + 16 * half + slot])
                term = part[:, j * 128 : (j + 1) * 128]
                total[:, here] = term if half == 0 else total[:, here] + term
                slot += 1
    if steps == (0,):
        outs[0][...] = total[...] + wide
    else:
        size = outs[0].shape[0]
        for g, out in enumerate(outs):
            out[...] = total[g * size : (g + 1) * size, :].astype(BF16)


def token_parts(steps, x, chips, gain, tokens, parts):
    count = len(steps)
    hbm = pl.BlockSpec(memory_space=pl.ANY)
    pieces = 1 if steps == (0,) else 2
    kind = F32 if steps == (0,) else BF16
    vmem = pl.BlockSpec(memory_space=pltpu.VMEM)
    smem = pl.BlockSpec(memory_space=pltpu.SMEM)
    return pl.pallas_call(
        functools.partial(token_kernel, steps),
        out_shape=[jax.ShapeDtypeStruct((count * 128 // pieces, 2048), kind)] * pieces,
        in_specs=[smem, smem]
        + [vmem] * (1 + count + 5)
        + [hbm]
        + [vmem] * EARLY
        + [hbm] * (len(parts) - 6 - EARLY),
        out_specs=[vmem] * pieces,
        scratch_shapes=[
            pltpu.VMEM((count * 128, 2048), BF16),
            pltpu.VMEM((2, count * 128, 2048), BF16),
            pltpu.VMEM((count * 128, 2048), F32),
            pltpu.VMEM((1024, 2048), BF16),
            pltpu.VMEM((32 - 12, 2, 128, 512), BF16),
            pltpu.SemaphoreType.DMA((2,)),
        ],
        cost_estimate=pl.CostEstimate(
            flops=count * 128 * 2048 * 3072 * 2, bytes_accessed=12 * 2**20, transcendentals=0
        ),
        compiler_params=pltpu.CompilerParams(vmem_limit_bytes=34 * 2**20),
        name="token_parts",
    )(x, chips, gain, *tokens, *parts)


def ring_pairs(axis, step):
    pairs = []
    for z in range(4):
        for y in range(4):
            for core in range(2):
                if (axis == 1) == (core == 0):
                    to = z * 4 + (y + step) % 4
                else:
                    to = (z + step) % 4 * 4 + y
                pairs.append(((z * 4 + y) * 2 + core, to * 2 + core))
    return pairs


PAIRS = {(axis, step): ring_pairs(axis, step) for axis in (1, 2) for step in (1, -1)}


def passed(array, axis, step):
    return lax.ppermute(array, SEQ, PAIRS[axis, step])


def source_chip(a, b, core=0):
    z, y = lax.axis_index("z"), lax.axis_index("y")
    first = lax.axis_index("c") == core
    dz, dy = jnp.where(first, b, a), jnp.where(first, a, b)
    return (z + dz + 4) % 4 * 4 + (y + dy + 4) % 4


def per_device(
    tokens,
    queries,
    keys,
    values,
    lambdas,
    head_gain,
    out_weight,
    mixer_gain,
    up_weight,
    down_weight,
):
    core = lax.axis_index("c")
    chip = lax.axis_index("z") * 4 + lax.axis_index("y")
    first = core == 0
    swap = [(0, 1), (1, 0)]

    def along_x(array, step):
        return lax.ppermute(array, "x", [(i, (i + step) % 4) for i in range(4)])

    def swapped(array):
        return lax.ppermute(array, "c", swap)

    def packed(head):
        cols = slice(head * DV, (head + 1) * DV)
        k = keys[:, cols].reshape(4, DV, DV)
        v = values[:, cols].reshape(4, DV, DV)
        q = queries[:, cols].reshape(4, DV, DV)
        return jnp.concatenate([k, jnp.swapaxes(v, 1, 2), q], axis=0)

    head_a, head_b = packed(0), packed(1)
    keep = jnp.where(first, head_a, head_b)
    other = swapped(jnp.where(first, head_b, head_a))
    even, odd = jnp.where(first, keep, other), jnp.where(first, other, keep)
    chunk = jnp.stack([even[:8], odd[:8]])

    def flat(chip_id, core_id):
        return chip_id * 2 + core_id

    high = lax.ppermute(odd[8:], ("z", "y"), [(i, 15 - i) for i in range(16)])
    query = jnp.concatenate([even[8:].reshape(HALF, DV), high.reshape(HALF, DV)], axis=0).T
    query = query * jnp.asarray(DQK ** (-0.5), BF16)
    none = jnp.zeros((DQK, 2 * HALF), BF16)
    query = jnp.stack(
        [
            jnp.concatenate([query[:DQK], none], axis=0),
            jnp.concatenate([none, query[DQK:]], axis=0),
        ]
    )

    lam = jnp.where(first, lambdas[0:1], lambdas[1:2])
    gain = head_gain[None]

    near = (0, -1, 1, 2)
    order = [(a, b) for b in (0, -1, 1, 2) for a in near]
    offsets = [jnp.asarray([p[n] for p in order], jnp.int32) for n in range(2)]
    table = jnp.concatenate(
        [chip[None]] + [source_chip(*offsets, core) for core in (0, 1)]
    ).astype(jnp.int32)

    def attending(slots, state, edge=None, last=False):
        places = [p for place, _ in slots for p in (place if isinstance(place[0], tuple) else (place,))]
        at = tuple(1 + order.index(place) for place in places)
        return attend([c for _, c in slots], at, table, lam, query, gain, state, edge, last)

    near_p, near_n = passed(chunk, 1, 1), passed(chunk, 1, -1)
    state = attending([((0, 0), chunk)], None, "own")
    across = passed(near_p, 1, 1)
    pair_a = jnp.stack([chunk, near_p])
    a_p, a_n = passed(pair_a, 2, 1), passed(pair_a, 2, -1)
    pair_b = jnp.stack([near_n, across])
    b_p, b_n = passed(pair_b, 2, 1), passed(pair_b, 2, -1)
    over_p = passed(a_p, 2, 1)
    state = attending(
        [
            ((-1, 0), near_p),
            ((1, 0), near_n),
            ((2, 0), across),
            (((0, -1), (-1, -1)), a_p),
            (((0, 1), (-1, 1)), a_n),
        ],
        state,
        "other",
    )
    over_n = passed(b_n, 2, -1)
    state = attending([(((1, -1), (2, -1)), b_p), (((1, 1), (2, 1)), b_n)], state, "other")

    tokens_p, tokens_n = along_x(tokens, 1), along_x(tokens, -1)
    tokens_far = along_x(tokens_p, 1)
    both = jnp.stack([up_weight, down_weight.T])
    both_a, both_b = both[:, :, :512], both[:, :, 512:]
    keep = jnp.where(first, both_a, both_b)
    other = swapped(jnp.where(first, both_b, both_a))
    unit = jnp.concatenate(
        [jnp.where(first, keep, other), jnp.where(first, other, keep)], axis=1
    )
    unit_p, unit_n = passed(unit, 1, 1), passed(unit, 1, -1)
    unit_f = passed(unit_p, 1, 1)
    row = jnp.stack([unit, unit_p, unit_n, unit_f])
    row_p, row_n = passed(row, 2, 1), passed(row, 2, -1)
    row_a, row_b = passed(row_p[:2], 2, 1), passed(row_n[2:], 2, -1)
    weights = [row, row_p, row_n, row_a, row_b]
    weights += [swapped(w) for w in weights]
    low, high = attending(
        [(((0, 2), (-1, 2)), over_p), (((1, 2), (2, 2)), over_n)], state, last=True
    )

    back = [(flat(i, 1), flat(i, 0)) for i in range(16)] + [
        (flat(i, 0), flat(15 - i, 1)) for i in range(16)
    ]
    flip = [(flat(i, 1), flat(15 - i, 1)) for i in range(16)]
    got_far = lax.ppermute(high, SEQ, flip)
    got = lax.ppermute(jnp.where(first, high, low), SEQ, back)
    attended = jnp.concatenate([jnp.where(first, low, got), jnp.where(first, got, got_far)], axis=1)

    prev, following = along_x(attended, 1), along_x(attended, -1)
    far_top = along_x(prev[:256], 1)
    far_low = along_x(following[256:], -1)
    x = lax.axis_index("x")[None]
    parts = (attended, prev, following, far_top, far_low, out_weight, *weights)
    gain = mixer_gain[None]
    far_top_part, far_low_part = token_parts((2,), x, table, gain, (tokens_far,), parts)
    from_prev = along_x(far_top_part, 1)
    from_next = along_x(far_low_part, -1)
    prev_part, next_part = token_parts((3, 1), x, table, gain, (tokens_p, tokens_n), parts)

    def added(a, b):
        return (a.astype(F32) + b.astype(F32)).astype(BF16)

    none = jnp.zeros((64, 2048), BF16)
    to_next = added(next_part, jnp.concatenate([from_prev, none], axis=0))
    to_prev = added(prev_part, jnp.concatenate([none, from_next], axis=0))
    got_prev = along_x(to_next, 1)
    got_next = along_x(to_prev, -1)
    (total,) = token_parts((0,), x, table, gain, (tokens,), parts)
    return (total + got_prev.astype(F32) + got_next.astype(F32)).astype(BF16)


def solution(mesh):
    grid = Mesh(mesh.devices.reshape(4, 4, 2, 4), ("z", "y", "c", "x"))
    placed = (
        P((*SEQ, "x"), None),
        P(SEQ, "x"),
        P(SEQ, "x"),
        P(SEQ, "x"),
        P("x"),
        P(),
        P(),
        P(),
        P(SEQ, "x"),
        P("x", SEQ),
    )

    return jax.shard_map(
        per_device, mesh=grid, in_specs=placed, out_specs=P((*SEQ, "x"), None), check_vma=False
    )
```

```python
import functools

import jax
import jax.numpy as jnp
from jax import lax
from jax.experimental import pallas as pl
from jax.experimental.pallas import tpu as pltpu
from jax.sharding import Mesh, PartitionSpec as P


DQK = 64
DV = 128
HALF = 512
TILE = 256
BF16 = jnp.bfloat16
F32 = jnp.float32
NEG = -1e30
SEQ = ("z", "y", "c")


ROWS = DV + 16


def attend_kernel(spans, at, edge, last, ids_ref, lam_ref, q_ref, gain_ref, *refs):
    first = edge == "own"
    if not first:
        top_in, acc_in, *refs = refs
    pieces, refs = refs[: len(spans)], refs[len(spans) :]
    if last:
        low_ref, high_ref, tops, acc, *refs = refs
    else:
        tops, acc, *refs = refs
    held, sems, items, seen, scores_a, scores_b, peaks_a, peaks_b = refs
    own = ids_ref[0]
    slots = held.shape[0]
    slot = 0
    for piece, span in zip(pieces, spans):
        for j in range(span):
            pltpu.make_async_copy(piece.at[j], held.at[slot], sems.at[slot]).start()
            slot += 1
    if first:
        tops[...] = jnp.full(tops.shape, NEG, F32)
        acc[...] = jnp.zeros(acc.shape, F32)
    else:
        tops[...] = top_in[...]
        acc[...] = acc_in[...]

    seen[0] = 0

    units = [(t, m) for t in range(HALF // TILE) for m in range(2)]
    parts = 2 * HALF // TILE
    ones = jnp.ones((ROWS - DV, TILE), BF16)

    def columns(side, t):
        return pl.ds(pl.multiple_of(side * HALF, HALF) + t * TILE, TILE)

    def key_part(slot, j):
        return held[slot, j // 2, 2 * (j % 2) : 2 * (j % 2) + 2].reshape(TILE, DV)

    def value_part(slot, j):
        n = 4 + 2 * (j % 2)
        vals = jnp.concatenate([held[slot, j // 2, n], held[slot, j // 2, n + 1]], axis=1)
        return jnp.concatenate([vals, ones], axis=0)

    def score_steps(item, scores, peaks):
        slot, side = item // 2, item % 2
        for u, (t, m) in enumerate(units):
            peak = None
            for j in range(parts):
                s = jnp.dot(
                    key_part(slot, j), q_ref[m, :, columns(side, t)], preferred_element_type=F32
                )
                scores[u, j * TILE : (j + 1) * TILE, :] = s
                high = jnp.max(s.reshape(TILE // 8, 8, TILE), axis=0)
                peak = high if peak is None else jnp.maximum(peak, high)
                if j == parts - 1:
                    peaks[u] = peak
                yield

    def weight_steps(item, scores, peaks):
        slot, side = item // 2, item % 2
        for u, (t, m) in enumerate(units):
            cols = columns(side, t)
            old = tops[m, 0:1, cols]
            top = jnp.maximum(old, jnp.max(peaks[u], axis=0, keepdims=True))
            shrink = jnp.exp(old - top)
            tops[m, 0:1, cols] = top
            total = None
            for j in range(parts):
                p = jnp.exp(scores[u, j * TILE : (j + 1) * TILE, :] - top).astype(BF16)
                part = jnp.dot(value_part(slot, j), p, preferred_element_type=F32)
                total = part if total is None else total + part
                if j == parts - 1:
                    acc[m, :, cols] = acc[m, :, cols] * shrink + total
                yield

    def together(*steps):
        steps = list(steps)
        while steps:
            steps = [s for s in steps if next(s, True) is None]

    def listed():
        count = jnp.int32(0)
        for i in range(slots):
            for side, limit in ((0, own), (1, 15 - own)):
                items[count] = 2 * i + side
                count = count + (ids_ref[at[i]] < limit).astype(jnp.int32)
        return count

    def ready(item):
        def one(slot, carry):
            pltpu.make_async_copy(held.at[slot], held.at[slot], sems.at[slot]).wait()
            return carry

        lax.fori_loop(seen[0], item // 2 + 1, one, 0)
        seen[0] = jnp.maximum(seen[0], item // 2 + 1)

    def pair(k, carry):
        one, two, three = items[2 * k], items[2 * k + 1], items[2 * k + 2]
        ready(two)
        together(score_steps(two, scores_b, peaks_b), weight_steps(one, scores_a, peaks_a))

        @pl.when(2 * k + 1 < count)
        def _():
            ready(three)
            together(score_steps(three, scores_a, peaks_a), weight_steps(two, scores_b, peaks_b))

        return carry

    if not first:
        count = listed()
        items[count] = 0
        items[count + 1] = 0

        @pl.when(count > 0)
        def _():
            ready(items[0])
            together(score_steps(items[0], scores_a, peaks_a))

        lax.fori_loop(0, (count + 1) // 2, pair, 0)

    def edge_item(slot, side, allowed):
        def tile(t, carry):
            cols = pl.ds(pl.multiple_of(side * HALF + t * TILE, TILE), TILE)
            for m in range(2):
                for j in range(parts):
                    s = jnp.dot(key_part(slot, j), q_ref[m, :, cols], preferred_element_type=F32)
                    key_pos = lax.broadcasted_iota(jnp.int32, (TILE, TILE), 0) + j * TILE
                    query_pos = lax.broadcasted_iota(jnp.int32, (TILE, TILE), 1)
                    scores_a[m, j * TILE : (j + 1) * TILE, :] = jnp.where(
                        key_pos <= query_pos + (t * TILE + allowed), s, -jnp.inf
                    )
            for m in range(2):
                old = tops[m, 0:1, cols]
                top = jnp.maximum(old, jnp.max(scores_a[m], axis=0, keepdims=True))
                shrink = jnp.exp(old - top)
                tops[m, 0:1, cols] = top
                total = None
                for j in range(parts):
                    p = jnp.exp(scores_a[m, j * TILE : (j + 1) * TILE, :] - top).astype(BF16)
                    part = jnp.dot(value_part(slot, j), p, preferred_element_type=F32)
                    total = part if total is None else total + part
                acc[m, :, cols] = acc[m, :, cols] * shrink + total
            return carry

        lax.fori_loop(0, HALF // TILE, tile, 0)

    ready(2 * slots - 2)
    if edge == "own":


        def own_side(side, carry):
            edge_item(0, side, side * 2 * HALF)
            return carry

        lax.fori_loop(0, 1 + (own < 15 - own).astype(jnp.int32), own_side, 0)

    if edge == "other":

        here = jnp.int32(-1)
        for i in range(slots):
            here = jnp.where(ids_ref[at[i]] == 15 - own, i, here)

        @pl.when(here >= 0)
        def _():
            edge_item(here, 1, HALF)

    if last:
        for t in range(2 * HALF // TILE):
            cols = slice(t * TILE, (t + 1) * TILE)
            differ = acc[0, :DV, cols] / acc[0, DV : DV + 1, cols] - lam_ref[0] * (
                acc[1, :DV, cols] / acc[1, DV : DV + 1, cols]
            )
            spread = lax.rsqrt(jnp.mean(differ * differ, axis=0, keepdims=True) + 1e-06)
            out_ref = low_ref if t * TILE < HALF else high_ref
            rows = slice(t * TILE % HALF, t * TILE % HALF + TILE)
            out_ref[rows, :] = ((differ * spread).T * gain_ref[...]).astype(BF16)


def attend(slots, at, ids, lam, query, gain, state, edge, last):
    pieces = [p if p.ndim == 5 else p[None] for p in slots]
    spans = tuple(p.shape[0] for p in pieces)
    count = sum(spans)
    vmem = pl.BlockSpec(memory_space=pltpu.VMEM)
    smem = pl.BlockSpec(memory_space=pltpu.SMEM)
    held = [
        pltpu.VMEM((count, 2, 8, DV, DV), BF16),
        pltpu.SemaphoreType.DMA((count,)),
        pltpu.SMEM((2 * count + 2,), jnp.int32),
        pltpu.SMEM((1,), jnp.int32),
        pltpu.VMEM((4, 2 * HALF, TILE), F32),
        pltpu.VMEM((4, 2 * HALF, TILE), F32),
        pltpu.VMEM((4, 8, TILE), F32),
        pltpu.VMEM((4, 8, TILE), F32),
    ]
    shapes = [(2, 8, 2 * HALF), (2, ROWS, 2 * HALF)]
    if last:
        out_shape = (jax.ShapeDtypeStruct((HALF, DV), BF16),) * 2
        scratch = [pltpu.VMEM(s, F32) for s in shapes] + held
        out_specs = (vmem, vmem)
    else:
        out_shape = tuple(jax.ShapeDtypeStruct(s, F32) for s in shapes)
        scratch = held
        out_specs = (vmem, vmem)
    state = [] if state is None else list(state)
    flops = count * 2 * HALF * HALF * 2 * 2 * 2 * (DV + DV) // 2
    return pl.pallas_call(
        functools.partial(attend_kernel, spans, at, edge, last),
        out_shape=out_shape,
        in_specs=[smem, smem, vmem, vmem]
        + [vmem] * len(state)
        + [pl.BlockSpec(memory_space=pl.ANY)] * len(pieces),
        out_specs=out_specs,
        scratch_shapes=scratch,
        cost_estimate=pl.CostEstimate(
            flops=flops, bytes_accessed=count * 2**19, transcendentals=count * 2**20
        ),
        compiler_params=pltpu.CompilerParams(vmem_limit_bytes=26 * 2**20),
        name="attend",
    )(ids, lam, query, gain, *state, *pieces)


def square_relu(x):
    x = jnp.maximum(x, 0.0)
    return (x * x).astype(BF16)


CUTS = 8


def token_kernel(steps, x_ref, chips_ref, gain_ref, *refs):
    tokens_refs, refs = refs[: len(steps)], refs[len(steps) :]
    heads_refs, proj_ref, refs = refs[:5], refs[5], refs[6:]
    weight_refs, refs = refs[:10], refs[10:]
    outs, (heads, tokens, proj, up, down, sems) = refs[:-6], refs[-6:]
    x = x_ref[0]

    def copied(source, target, n):
        pltpu.make_async_copy(source, target, sems.at[n]).start()

    def settled(target, n):
        pltpu.make_async_copy(target, target, sems.at[n]).wait()

    for g, step in enumerate(steps):
        who = (x + step) % 4
        rows = pl.ds(pl.multiple_of(who * 128, 128), 128)
        here = pl.ds(g * 128, 128)
        copied(tokens_refs[g], tokens.at[here], 1)
        for back, source in zip((0, 3, 1), heads_refs):
            cols = pl.ds(pl.multiple_of((x + back) % 4 * 256, 256), 256)
            copied(source.at[rows], heads.at[here, cols], 0)
        cols = pl.ds(pl.multiple_of((x + 2) % 4 * 256, 256), 256)
        half = pl.ds(pl.multiple_of(who % 2 * 128, 128), 128)

        @pl.when(who < 2)
        def _(half=half, here=here, cols=cols):
            copied(heads_refs[3].at[half], heads.at[here, cols], 0)

        @pl.when(who >= 2)
        def _(half=half, here=here, cols=cols):
            copied(heads_refs[4].at[half], heads.at[here, cols], 0)

    for n in range(CUTS):
        part = pl.ds(n * 1024 // CUTS, 1024 // CUTS)
        copied(proj_ref.at[part], proj.at[part], 2)
    for kind, target in enumerate((up, down)):
        for half in range(2):
            slot = 0
            for piece in weight_refs[5 * half : 5 * half + 5]:
                for j in range(piece.shape[0]):
                    copied(
                        piece.at[j, kind], target.at[half, chips_ref[1 + 16 * half + slot]], 3 + kind
                    )
                    slot += 1

    settled(heads, 0)
    settled(tokens, 1)
    settled(proj, 2)
    projected = jnp.dot(heads[...], proj[...], preferred_element_type=F32).astype(BF16)
    resid = (tokens[...].astype(F32) + projected.astype(F32)).astype(BF16)
    wide = resid.astype(F32)
    spread = lax.rsqrt(jnp.mean(wide * wide, axis=1, keepdims=True) + 1e-06)
    tokens[...] = resid
    normed = (wide * spread * gain_ref[...]).astype(BF16)
    settled(up, 3)
    made = [
        square_relu(
            jnp.dot(normed, up[half].reshape(2048, 512), preferred_element_type=F32)
        )
        for half in range(2)
    ]
    settled(down, 4)
    for n in range(0, 2048, 512):
        cols = slice(n, n + 512)
        part = None
        for half in range(2):
            term = lax.dot_general(
                made[half],
                down[half, n // 128 : n // 128 + 4].reshape(512, 512),
                (((1,), (1,)), ((), ())),
                preferred_element_type=F32,
            )
            part = term if part is None else part + term
        if steps == (0,):
            outs[0][:, cols] = part + tokens[:, cols].astype(F32)
        else:
            size = outs[0].shape[0]
            for g, out in enumerate(outs):
                out[:, cols] = part[g * size : (g + 1) * size].astype(BF16)


def token_parts(steps, x, chips, gain, tokens, parts):
    count = len(steps)
    pieces = 1 if steps == (0,) else 2
    kind = F32 if steps == (0,) else BF16
    vmem = pl.BlockSpec(memory_space=pltpu.VMEM)
    smem = pl.BlockSpec(memory_space=pltpu.SMEM)
    return pl.pallas_call(
        functools.partial(token_kernel, steps),
        out_shape=[jax.ShapeDtypeStruct((count * 128 // pieces, 2048), kind)] * pieces,
        in_specs=[smem, smem, vmem]
        + [pl.BlockSpec(memory_space=pl.ANY)] * (count + len(parts)),
        out_specs=[vmem] * pieces,
        scratch_shapes=[
            pltpu.VMEM((count * 128, 1024), BF16),
            pltpu.VMEM((count * 128, 2048), BF16),
            pltpu.VMEM((1024, 2048), BF16),
            pltpu.VMEM((2, 16, 128, 512), BF16),
            pltpu.VMEM((2, 16, 128, 512), BF16),
            pltpu.SemaphoreType.DMA((5,)),
        ],
        cost_estimate=pl.CostEstimate(
            flops=count * 128 * 2048 * 3072 * 2, bytes_accessed=12 * 2**20, transcendentals=0
        ),
        compiler_params=pltpu.CompilerParams(
            vmem_limit_bytes=(61 if steps == (2,) else 44) * 2**20
        ),
        name="token_parts",
    )(x, chips, gain, *tokens, *parts)


def ring_pairs(axis, step):
    pairs = []
    for z in range(4):
        for y in range(4):
            for core in range(2):
                if (axis == 1) == (core == 0):
                    to = z * 4 + (y + step) % 4
                else:
                    to = (z + step) % 4 * 4 + y
                pairs.append(((z * 4 + y) * 2 + core, to * 2 + core))
    return pairs


PAIRS = {(axis, step): ring_pairs(axis, step) for axis in (1, 2) for step in (1, -1)}


def passed(array, axis, step):
    return lax.ppermute(array, SEQ, PAIRS[axis, step])


def source_chip(a, b, core=0):
    z, y = lax.axis_index("z"), lax.axis_index("y")
    first = lax.axis_index("c") == core
    dz, dy = jnp.where(first, b, a), jnp.where(first, a, b)
    return (z + dz + 4) % 4 * 4 + (y + dy + 4) % 4


def per_device(
    tokens,
    queries,
    keys,
    values,
    lambdas,
    head_gain,
    out_weight,
    mixer_gain,
    up_weight,
    down_weight,
):
    core = lax.axis_index("c")
    chip = lax.axis_index("z") * 4 + lax.axis_index("y")
    first = core == 0
    swap = [(0, 1), (1, 0)]

    def along_x(array, step):
        return lax.ppermute(array, "x", [(i, (i + step) % 4) for i in range(4)])

    def swapped(array):
        return lax.ppermute(array, "c", swap)

    def packed(head):
        cols = slice(head * DV, (head + 1) * DV)
        k = keys[:, cols].reshape(4, DV, DV)
        v = values[:, cols].reshape(4, DV, DV)
        q = queries[:, cols].reshape(4, DV, DV)
        return jnp.concatenate([k, jnp.swapaxes(v, 1, 2), q], axis=0)

    head_a, head_b = packed(0), packed(1)
    keep = jnp.where(first, head_a, head_b)
    other = swapped(jnp.where(first, head_b, head_a))
    even, odd = jnp.where(first, keep, other), jnp.where(first, other, keep)
    chunk = jnp.stack([even[:8], odd[:8]])

    def flat(chip_id, core_id):
        return chip_id * 2 + core_id

    high = lax.ppermute(odd[8:], ("z", "y"), [(i, 15 - i) for i in range(16)])
    query = jnp.concatenate([even[8:].reshape(HALF, DV), high.reshape(HALF, DV)], axis=0).T
    query = query * jnp.asarray(DQK ** (-0.5), BF16)
    none = jnp.zeros((DQK, 2 * HALF), BF16)
    query = jnp.stack(
        [
            jnp.concatenate([query[:DQK], none], axis=0),
            jnp.concatenate([none, query[DQK:]], axis=0),
        ]
    )

    lam = jnp.where(first, lambdas[0:1], lambdas[1:2])
    gain = head_gain[None]

    near = (0, -1, 1, 2)
    order = [(a, b) for b in (0, -1, 1, 2) for a in near]
    offsets = [jnp.asarray([p[n] for p in order], jnp.int32) for n in range(2)]
    table = jnp.concatenate(
        [chip[None]] + [source_chip(*offsets, core) for core in (0, 1)]
    ).astype(jnp.int32)

    def attending(slots, state, edge=None, last=False):
        places = [p for place, _ in slots for p in (place if isinstance(place[0], tuple) else (place,))]
        at = tuple(1 + order.index(place) for place in places)
        return attend([c for _, c in slots], at, table, lam, query, gain, state, edge, last)

    near_p, near_n = passed(chunk, 1, 1), passed(chunk, 1, -1)
    state = attending([((0, 0), chunk)], None, "own")
    across = passed(near_p, 1, 1)
    pair_a = jnp.stack([chunk, near_p])
    a_p, a_n = passed(pair_a, 2, 1), passed(pair_a, 2, -1)
    pair_b = jnp.stack([near_n, across])
    b_p, b_n = passed(pair_b, 2, 1), passed(pair_b, 2, -1)
    over_p = passed(a_p, 2, 1)
    state = attending(
        [
            ((-1, 0), near_p),
            ((1, 0), near_n),
            ((2, 0), across),
            (((0, -1), (-1, -1)), a_p),
            (((0, 1), (-1, 1)), a_n),
        ],
        state,
        "other",
    )
    over_n = passed(b_n, 2, -1)
    state = attending([(((1, -1), (2, -1)), b_p), (((1, 1), (2, 1)), b_n)], state, "other")

    tokens_p, tokens_n = along_x(tokens, 1), along_x(tokens, -1)
    tokens_far = along_x(tokens_p, 1)
    both = jnp.stack([up_weight, down_weight.T])
    both_a, both_b = both[:, :, :512], both[:, :, 512:]
    keep = jnp.where(first, both_a, both_b)
    other = swapped(jnp.where(first, both_b, both_a))
    unit = jnp.concatenate(
        [jnp.where(first, keep, other), jnp.where(first, other, keep)], axis=1
    )
    unit_p, unit_n = passed(unit, 1, 1), passed(unit, 1, -1)
    unit_f = passed(unit_p, 1, 1)
    row = jnp.stack([unit, unit_p, unit_n, unit_f])
    row_p, row_n = passed(row, 2, 1), passed(row, 2, -1)
    row_a, row_b = passed(row_p[:2], 2, 1), passed(row_n[2:], 2, -1)
    weights = [row, row_p, row_n, row_a, row_b]
    weights += [swapped(w) for w in weights]
    low, high = attending(
        [(((0, 2), (-1, 2)), over_p), (((1, 2), (2, 2)), over_n)], state, last=True
    )

    back = [(flat(i, 1), flat(i, 0)) for i in range(16)] + [
        (flat(i, 0), flat(15 - i, 1)) for i in range(16)
    ]
    flip = [(flat(i, 1), flat(15 - i, 1)) for i in range(16)]
    got_far = lax.ppermute(high, SEQ, flip)
    got = lax.ppermute(jnp.where(first, high, low), SEQ, back)
    attended = jnp.concatenate([jnp.where(first, low, got), jnp.where(first, got, got_far)], axis=1)

    prev, following = along_x(attended, 1), along_x(attended, -1)
    far_top = along_x(prev[:256], 1)
    far_low = along_x(following[256:], -1)
    x = lax.axis_index("x")[None]
    parts = (attended, prev, following, far_top, far_low, out_weight, *weights)
    gain = mixer_gain[None]
    far_top_part, far_low_part = token_parts((2,), x, table, gain, (tokens_far,), parts)
    from_prev = along_x(far_top_part, 1)
    from_next = along_x(far_low_part, -1)
    prev_part, next_part = token_parts((3, 1), x, table, gain, (tokens_p, tokens_n), parts)

    def added(a, b):
        return (a.astype(F32) + b.astype(F32)).astype(BF16)

    none = jnp.zeros((64, 2048), BF16)
    to_next = added(next_part, jnp.concatenate([from_prev, none], axis=0))
    to_prev = added(prev_part, jnp.concatenate([none, from_next], axis=0))
    got_prev = along_x(to_next, 1)
    got_next = along_x(to_prev, -1)
    (total,) = token_parts((0,), x, table, gain, (tokens,), parts)
    return (total + got_prev.astype(F32) + got_next.astype(F32)).astype(BF16)


def solution(mesh):
    grid = Mesh(mesh.devices.reshape(4, 4, 2, 4), ("z", "y", "c", "x"))
    placed = (
        P((*SEQ, "x"), None),
        P(SEQ, "x"),
        P(SEQ, "x"),
        P(SEQ, "x"),
        P("x"),
        P(),
        P(),
        P(),
        P(SEQ, "x"),
        P("x", SEQ),
    )

    return jax.shard_map(
        per_device, mesh=grid, in_specs=placed, out_specs=P((*SEQ, "x"), None), check_vma=False
    )
```
